32 devices in a mesh: grp: 2 (over y), ep: 8 (over z, core), tp: 2 (over x).
Axes of the slice: x: 2, y: 2, z: 4, core: 2. Of those that a mesh axis runs over, the one named last changes fastest.
Arguments:
- mixer_tokens: bfloat16 [4096, 2048], P(('grp', 'ep', 'tp')), parts along dimension 0, may hold values from -6 to 6
- mixer_gain: float32 [2048], replicated, may hold values from 0.1 to 1.9
- proj_in: bfloat16 [2048, 1024], P(None, 'tp'), may hold values from -0.125 to 0.125
- pool_weight: bfloat16 [4, 256, 256], P('tp'), may hold values from -0.375 to 0.375
- pool_scale: float32 [1024], P('tp'), may hold values from 0.1 to 1.9
- proj_out: bfloat16 [1024, 2048], P('tp'), may hold values from -0.1875 to 0.1875
- expert_tokens: bfloat16 [4096, 2048], P(('grp', 'ep', 'tp')), parts along dimension 0, may hold values from -6 to 6
- expert_gain: float32 [2048], replicated, may hold values from 0.1 to 1.9
- expert_route: int32 [4096, 2], P(('grp', 'ep')), parts along dimension 0, may hold values from 0 to 15, as said below
- route_gate: float32 [4096, 2], P(('grp', 'ep')), parts along dimension 0, may hold values from 0.1 to 1
- expert_gate: bfloat16 [16, 2048, 1024], P('ep', None, 'tp'), may hold values from -0.125 to 0.125
- expert_up: bfloat16 [16, 2048, 1024], P('ep', None, 'tp'), may hold values from -0.125 to 0.125
- expert_down: bfloat16 [16, 1024, 2048], P('ep', 'tp'), may hold values from -0.1875 to 0.1875
Outputs:
- mixed_rows: bfloat16 [4096, 2048], P(('grp', 'ep', 'tp')), parts along dimension 0
- moe_rows: bfloat16 [4096, 2048], P(('grp', 'ep', 'tp')), parts along dimension 0
The draws below stay inside these ranges and needn't reach their ends.
There are 2 independent parts, one for each index of `grp`. The reference program is written for one: setup_inputs(seed, part) draws one part's arguments, and reference() takes and returns one part's arrays. A program takes and returns all parts, laid end to end along the dimension named above; an argument that names none is the same for every part. Nothing has to cross between parts.
Inputs may be any that keep to these rules, and one draw needn't show every extreme that they name: `expert_route`: each row names two different experts of one group of 4 consecutive experts. In each aligned block of 128 rows (the routes of the tokens that lie on one device) no expert is named by more than 32 rows, and every expert of a group that the block names at all is named by exactly 32 of its rows; one group, the same in every block, is named in every block, and which other groups a block names varies from block to block.
All inputs are finite; a program needn't handle non-finite values.
Results may differ from the reference program's by a relative error of at most 0.011.
Values may be sent and summed in bfloat16 or wider, within the bound.
A program may use at most 128 MiB of HBM per device.

```python
import jax
import jax.numpy as jnp
from jax import lax

D = 2048
POOL_WIDTH = 1024
POOL_GROUPS = 4
HIDDEN_SIZE = 1024
GROUP_SIZE = 4
TOK_DEV = 128
EXPERTS = 16
GROUPS = 4
CAP = 32
TOKENS = 2048
N_EP = 8
N_TP = 2


def draw_expert_route(key, part):
    blocks = TOKENS // TOK_DEV
    unit = TOK_DEV // GROUPS
    hot_key, cold_key, label_key, order_key = jax.random.split(jax.random.fold_in(key, 17), 4)
    hot_group = jax.random.randint(hot_key, (), 0, GROUPS)
    cold_keys = jax.random.split(cold_key, blocks)
    cold_order = jax.vmap(lambda single: jax.random.permutation(single, GROUPS - 1))(cold_keys).astype(jnp.int32)
    position = jnp.arange(TOK_DEV, dtype=jnp.int32)
    unit_index = position // unit
    within = position % unit
    pair_index = jnp.maximum((unit_index - 2) // 2, 0)
    cold_pick = jnp.take_along_axis(cold_order, jnp.broadcast_to(pair_index[None, :], (blocks, TOK_DEV)), axis=1)
    group_id = jnp.where(unit_index[None, :] < 2, hot_group, (hot_group + 1 + cold_pick) % GROUPS)
    member = unit_index % 2 * unit + within
    first_pick = member % GROUP_SIZE
    second_pick = (member + 1) % GROUP_SIZE
    label_keys = jax.random.split(label_key, blocks * GROUPS)
    labels = jax.vmap(lambda single: jax.random.permutation(single, GROUP_SIZE))(label_keys).reshape(blocks, GROUPS, GROUP_SIZE).astype(jnp.int32)
    group_labels = jnp.take_along_axis(labels, group_id[:, :, None], axis=1)
    first_label = jnp.take_along_axis(group_labels, jnp.broadcast_to(first_pick[None, :, None], (blocks, TOK_DEV, 1)), axis=2)[:, :, 0]
    second_label = jnp.take_along_axis(group_labels, jnp.broadcast_to(second_pick[None, :, None], (blocks, TOK_DEV, 1)), axis=2)[:, :, 0]
    routes = jnp.stack([group_id * GROUP_SIZE + first_label, group_id * GROUP_SIZE + second_label], axis=-1)
    order_keys = jax.random.split(order_key, blocks)
    orders = jax.vmap(lambda single: jax.random.permutation(single, TOK_DEV))(order_keys).astype(jnp.int32)
    shuffled = jnp.take_along_axis(routes, jnp.broadcast_to(orders[:, :, None], (blocks, TOK_DEV, 2)), axis=1)
    return shuffled.reshape(TOKENS, 2).astype(jnp.int32)


def steps_of(rng, extent, shards, low, top_value):
    gain = 1.0
    for dim, blocks in shards:
        steps = jax.random.uniform(jax.random.fold_in(jax.random.fold_in(rng, 6), dim), (blocks,), jnp.float32, low / len(shards), top_value / len(shards))
        gain = gain * jnp.repeat(jnp.exp(steps), extent[dim] // blocks).reshape((-1,) + (1,) * (len(extent) - 1 - dim))
    return gain


def scatter_about(key, dims, width, most, cuts=(), kind=jnp.bfloat16):
    drawn = jax.random.normal(key, dims, jnp.float32) * width
    if len(cuts) > 0:
        drawn = steps_of(key, dims, cuts, -0.22, 0.18) * drawn
    return jnp.clip(drawn, min=-most, max=most).astype(kind)


def setup_inputs(seed: int = 0, part: int = 0) -> dict:
    streams_of = jax.random.split(jax.random.key(seed), 14)
    own_keys = jax.random.split(jax.random.fold_in(streams_of[13], part), 14)
    mixer_tokens = scatter_about(own_keys[0], (TOKENS, D), 1.0, 6.0, ((0, 16),))
    mixer_gain = jnp.clip(1.0 + 0.18 * jax.random.normal(streams_of[1], (D,), jnp.float32), 0.1, 1.9)
    proj_in = scatter_about(streams_of[2], (D, POOL_WIDTH), D ** -0.5, 0.125, ((1, 2),))
    pool_weight = scatter_about(streams_of[3], (POOL_GROUPS, POOL_WIDTH // POOL_GROUPS, POOL_WIDTH // POOL_GROUPS), (POOL_WIDTH // POOL_GROUPS) ** -0.5, 0.375, ((0, 2),))
    pool_scale = jnp.clip(1.0 + 0.18 * jax.random.normal(streams_of[4], (POOL_WIDTH,), jnp.float32), 0.1, 1.9)
    proj_out = scatter_about(streams_of[5], (POOL_WIDTH, D), POOL_WIDTH ** -0.5, 0.1875, ((0, 2),))
    expert_tokens = scatter_about(own_keys[6], (TOKENS, D), 1.0, 6.0, ((0, 16),))
    expert_gain = jnp.clip(1.0 + 0.18 * jax.random.normal(streams_of[7], (D,), jnp.float32), 0.1, 1.9)
    expert_route = draw_expert_route(jax.random.fold_in(jax.random.fold_in(streams_of[13], part), 71), part)
    route_gate = jnp.clip(0.1 + 0.9 * jax.random.uniform(own_keys[9], (TOKENS, 2), jnp.float32) ** steps_of(own_keys[9], (TOKENS, 2), ((0, 8),), -0.2, 0.2), 0.1, 1.0)
    expert_gate = scatter_about(streams_of[10], (EXPERTS, D, HIDDEN_SIZE), D ** -0.5, 0.125, ((0, 8), (2, 2)))
    expert_up = scatter_about(streams_of[11], (EXPERTS, D, HIDDEN_SIZE), D ** -0.5, 0.125, ((0, 8), (2, 2)))
    expert_down = scatter_about(streams_of[12], (EXPERTS, HIDDEN_SIZE, D), HIDDEN_SIZE ** -0.5, 0.1875, ((0, 8), (1, 2)))
    return dict(mixer_tokens=mixer_tokens, mixer_gain=mixer_gain, proj_in=proj_in, pool_weight=pool_weight, pool_scale=pool_scale, proj_out=proj_out, expert_tokens=expert_tokens, expert_gain=expert_gain, expert_route=expert_route, route_gate=route_gate, expert_gate=expert_gate, expert_up=expert_up, expert_down=expert_down)


norm_eps = 1e-05
rim_rows = 15

def layer_norm(values, norm_gain):
    widened = values.astype(jnp.float32)
    center = lax.optimization_barrier(jnp.mean(widened, axis=-1, keepdims=True))
    spread = lax.optimization_barrier(jnp.mean(jnp.square(widened - center), axis=-1, keepdims=True))
    return ((widened - center) * lax.rsqrt(spread + norm_eps) * norm_gain).astype(jnp.bfloat16)

def pooled_diff(extended, windows, first_row):
    widened = extended.astype(jnp.float32)
    row_total = widened.shape[0] - rim_rows
    own_rows = widened[rim_rows:]
    window_sum = own_rows
    for offset in range(1, rim_rows + 1):
        lagged = widened[rim_rows - offset:rim_rows - offset + row_total]
        window_sum = window_sum + jnp.where(offset < windows[None, :], lagged, 0.0)
    position = first_row + jnp.arange(row_total, dtype=jnp.int32)
    covered = jnp.minimum(position[:, None] + 1, windows[None, :]).astype(jnp.float32)
    return (window_sum / covered - own_rows).astype(jnp.bfloat16)

def reference(mixer_tokens, mixer_gain, proj_in, pool_weight, pool_scale, proj_out, expert_tokens, expert_gain, expert_route, route_gate, expert_gate, expert_up, expert_down):
    mixer_norm = layer_norm(mixer_tokens, mixer_gain)
    projected = jnp.dot(mixer_norm, proj_in, preferred_element_type=jnp.float32).astype(jnp.bfloat16)
    group_width = POOL_WIDTH // POOL_GROUPS
    channel = jnp.arange(POOL_WIDTH, dtype=jnp.int32)
    windows = jnp.left_shift(jnp.full_like(channel, 2), channel // group_width)
    extended = jnp.concatenate([jnp.zeros((rim_rows, POOL_WIDTH), jnp.bfloat16), projected], axis=0)
    differences = pooled_diff(extended, windows, 0)
    grouped = differences.astype(jnp.float32).reshape(TOKENS, POOL_GROUPS, group_width)
    pool_mixed = jnp.einsum('tgc,gcd->tgd', grouped, pool_weight.astype(jnp.float32))
    pooled = (pool_mixed.reshape(TOKENS, POOL_WIDTH) * pool_scale).astype(jnp.bfloat16)
    block_width = POOL_WIDTH // N_TP
    out_total = jnp.zeros((TOKENS, D), jnp.float32)
    for block in range(N_TP):
        out_part = jnp.dot(pooled[:, block * block_width:(block + 1) * block_width], proj_out[block * block_width:(block + 1) * block_width], preferred_element_type=jnp.float32)
        out_total = out_total + lax.optimization_barrier(out_part.astype(jnp.bfloat16)).astype(jnp.float32)
    mixed_rows = out_total.astype(jnp.bfloat16)
    expert_norm = layer_norm(expert_tokens, expert_gain)
    flat_route = expert_route.reshape(-1).astype(jnp.int32)
    flat_gate = route_gate.reshape(-1)
    limit = N_EP * N_TP * CAP
    quarter = HIDDEN_SIZE // N_TP

    def expert_pass(carry, expert):
        chosen = flat_route == expert
        found = jnp.nonzero(chosen, size=limit, fill_value=0)[0].astype(jnp.int32)
        valid = jnp.arange(limit, dtype=jnp.int32) < jnp.sum(chosen.astype(jnp.int32))
        token_index = found // 2
        picked = expert_norm[token_index]
        gate_matrix = lax.dynamic_index_in_dim(expert_gate, expert, 0, keepdims=False)
        up_matrix = lax.dynamic_index_in_dim(expert_up, expert, 0, keepdims=False)
        down_matrix = lax.dynamic_index_in_dim(expert_down, expert, 0, keepdims=False)
        gate_part = jnp.dot(picked, gate_matrix, preferred_element_type=jnp.float32)
        up_part = jnp.dot(picked, up_matrix, preferred_element_type=jnp.float32)
        hidden = (jax.nn.silu(gate_part) * up_part).astype(jnp.bfloat16)
        summed = jnp.zeros((limit, D), jnp.float32)
        for block in range(N_TP):
            down_part = jnp.dot(hidden[:, block * quarter:(block + 1) * quarter], down_matrix[block * quarter:(block + 1) * quarter], preferred_element_type=jnp.float32)
            summed = summed + lax.optimization_barrier(down_part.astype(jnp.bfloat16)).astype(jnp.float32)
        expert_out = lax.optimization_barrier(summed.astype(jnp.bfloat16)).astype(jnp.float32)
        weight = jnp.where(valid, flat_gate[found], 0.0)
        carry = carry.at[token_index].add(weight[:, None] * expert_out)
        return (carry, None)
    moe_total, unused = lax.scan(expert_pass, jnp.zeros((TOKENS, D), jnp.float32), jnp.arange(EXPERTS, dtype=jnp.int32))
    moe_rows = moe_total.astype(jnp.bfloat16)
    return (mixed_rows, moe_rows)
```

```python
import functools

import jax
import jax.numpy as jnp
from jax import lax
from jax.experimental import pallas as pl
from jax.experimental.pallas import tpu as pltpu
from jax.sharding import PartitionSpec as P

GROUP_SIZE = 4
MARK = 128
HALO = 16

norm_eps = 1e-05
MESH = pl.DeviceIdType.MESH
f32, bf16 = jnp.float32, jnp.bfloat16


def norm_rows(src, gain, store, step=16):
    def body(i, _):
        rows = pl.ds(pl.multiple_of(i * step, step), step)
        v = src[rows, :].astype(f32)
        center = jnp.mean(v, axis=-1, keepdims=True)
        v = v - center
        spread = jnp.mean(jnp.square(v), axis=-1, keepdims=True)
        store(rows, (v * lax.rsqrt(spread + norm_eps) * gain[...]).astype(bf16))
        return 0

    lax.fori_loop(0, src.shape[0] // step, body, 0)


def kernel(
    dims,
    mixer, mgain, proj_in, pool_w, pool_s, proj_out,
    tokens, egain, route, gate, wgate, wup, wdown,
    mixed, moe,
    w_in, w_pool, w_out, w_g, w_u, w_d,
    aug, mark, out, xs, hid, po, rd, sx, rx, sz, ret,
    mx, ext, mo, mr,
    s_w, s_z, r_z, s_x, r_x, s_d, r_d, s_o, r_o, s_p, r_p, s_b, r_b,
    s_m, r_m, s_h, r_h, s_q, r_q,
):
    nz, duo, nx, slots, own, d = dims
    ep, x = lax.axis_index("ep"), lax.axis_index("tp")
    n_ep = nz * duo
    z, c = ep // duo, lax.rem(ep, duo)
    mate = z * duo + (duo - 1 - c)
    nxt, prv = lax.rem(ep + 1, n_ep), lax.rem(ep + n_ep - 1, n_ep)

    def xpeer(k):
        return lax.rem(x + k, nx)

    def zpeer(k):
        return lax.rem(z + k, nz)

    def remote(src, dst, ssem, rsem, e, t):
        return pltpu.make_async_remote_copy(
            src_ref=src, dst_ref=dst, send_sem=ssem, recv_sem=rsem,
            device_id={"ep": e, "tp": t}, device_id_type=MESH)

    loads = [
        pltpu.make_async_copy(a, b, s_w.at[i])
        for i, (a, b) in enumerate(
            [(proj_in, w_in), (pool_w, w_pool), (proj_out, w_out), (wgate, w_g), (wup, w_u), (wdown, w_d)])
    ]
    for cp in loads:
        cp.start()

    barrier = pltpu.get_barrier_semaphore()

    def greet(e, t):
        pl.semaphore_signal(barrier, inc=1, device_id={"ep": e, "tp": t}, device_id_type=MESH)

    for k in range(1, nz):
        greet(zpeer(k) * duo + c, x)
    for k in range(1, nx):
        greet(ep, xpeer(k))
    greet(mate, x)
    greet(nxt, x)
    greet(prv, x)

    def keep_tokens(rows, v):
        aug[rows, pl.ds(0, d)] = v

    norm_rows(tokens, egain, keep_tokens)
    base = pl.ds(pl.multiple_of(x * own, own), own)
    rt = route[base, :]
    gt = gate[base, :]
    lane = lax.broadcasted_iota(jnp.int32, (own, MARK), 1)
    r0, r1 = rt[:, 0:1], rt[:, 1:2]
    i0, i1 = lax.rem(r0, GROUP_SIZE), lax.rem(r1, GROUP_SIZE)
    g0, g1 = gt[:, 0:1], gt[:, 1:2]
    head = jnp.where(lane == i0, g0, 0.0) + jnp.where(lane == i1, g1, 0.0)
    tail = jnp.where(lane == i0 + GROUP_SIZE, g0, 0.0) + jnp.where(lane == i1 + GROUP_SIZE, g1, 0.0)
    rest = tail - tail.astype(bf16).astype(f32)
    aug[:, pl.ds(d, MARK)] = (head + rest).astype(bf16)
    member = (lane == r0 // GROUP_SIZE).astype(f32)
    row = lax.broadcasted_iota(jnp.int32, (own, own), 0)
    col = lax.broadcasted_iota(jnp.int32, (own, own), 1)
    before = jnp.dot((col < row).astype(f32).astype(bf16), member.astype(bf16), preferred_element_type=f32)
    place = jnp.sum(member * (before + (lane * slots).astype(f32)), axis=-1, keepdims=True).astype(jnp.int32)
    slot = lax.broadcasted_iota(jnp.int32, (own, nz * slots), 1)
    mark[...] = (slot == place).astype(f32).astype(bf16)
    packed = lax.dot_general(
        mark[...], aug[...], (((0,), (0,)), ((), ())), preferred_element_type=f32
    ).astype(bf16)
    out[...] = packed.reshape(nz, slots, d + MARK)

    pl.semaphore_wait(barrier, nz - 1 + nx - 1 + 3)

    def send_z(k):
        g = zpeer(nz - k)
        return remote(out.at[g], xs.at[z, c, x], s_z.at[k], r_z.at[z], g * duo + c, x)

    def fwd_x(k, j):
        zs = zpeer(k)
        return remote(xs.at[zs, c, x], xs.at[zs, c, x], s_x.at[k, j], r_x.at[zs, x], ep, xpeer(j))

    def fwd_d(k, j):
        zs, xp = zpeer(k), xpeer(j)
        return remote(xs.at[zs, c, xp], xs.at[zs, c, xp], s_d.at[k, j], r_d.at[zs, xp], mate, x)

    def pair(k):
        zs = zpeer(k)
        return remote(po.at[zs, duo - 1 - c], rd.at[zs], s_o.at[k], r_o.at[zs], mate, x)

    def sum_x(k, j):
        zs, xp = zpeer(k), xpeer(j)
        return remote(sx.at[zs, xp], rx.at[zs, x], s_p.at[k, j], r_p.at[zs, x], ep, xp)

    def back(k):
        zs = zpeer(k)
        return remote(sz.at[zs], ret.at[z], s_b.at[k], r_b.at[z], zs * duo + c, x)

    def mix_x(j):
        return remote(mx.at[x], mx.at[x], s_m.at[j], r_m.at[x], ep, xpeer(j))

    def rim():
        return remote(ext.at[pl.ds(nx * own, HALO)], ext.at[pl.ds(0, HALO)], s_h, r_h, nxt, x)

    def mix_out(j):
        xp = xpeer(j)
        return remote(mo.at[xp], mr.at[x], s_q.at[j], r_q.at[x], ep, xp)

    def arrived(dst, rsem):
        remote(dst, dst, s_h, rsem, ep, xpeer(1)).wait_recv()

    for k in range(1, nz):
        send_z(k).start()
    xs[z, c, x] = out[z]

    def keep_mixer(rows, v):
        mx[x, rows, :] = v

    norm_rows(mixer, mgain, keep_mixer)
    for j in range(1, nx):
        mix_x(j).start()

    def mixer_project():
        for j in range(1, nx):
            arrived(mx.at[xpeer(j)], r_m.at[xpeer(j)])
        loads[0].wait()
        rows = mx[...].reshape(nx * own, d)
        ext[pl.ds(HALO, nx * own), :] = jnp.dot(rows, w_in[...], preferred_element_type=f32).astype(bf16)
        rim().start()

    def mixer_finish():
        arrived(ext.at[pl.ds(0, HALO)], r_h)
        loads[1].wait()
        loads[2].wait()
        groups, width = w_pool.shape[0], w_pool.shape[1]
        rows = nx * own
        at = ep * rows + lax.broadcasted_iota(jnp.int32, (rows, width), 0)
        total = None
        for g in range(groups):
            cols = pl.ds(g * width, width)
            v = ext[:, cols].astype(f32)
            r = lax.broadcasted_iota(jnp.int32, v.shape, 0)
            v = jnp.where((r < HALO) & (ep == 0), 0.0, v)
            group = x * groups + g
            s, window, picked = v, 1, None
            for level in range(groups * nx):
                s = s + pltpu.roll(s, window, 0)
                window *= 2
                picked = s if picked is None else jnp.where(group == level, s, picked)
            w = lax.shift_left(jnp.int32(2), group)
            covered = jnp.minimum(at + 1, w).astype(f32)
            diff = (picked[HALO:] / covered - v[HALO:]).astype(bf16)
            m = jnp.dot(diff, w_pool[g], preferred_element_type=f32) * pool_s[:, cols]
            part = jnp.dot(m.astype(bf16), w_out[cols, :], preferred_element_type=f32)
            total = part if total is None else total + part
        mo[...] = total.astype(bf16).reshape(nx, own, d)
        for j in range(1, nx):
            mix_out(j).start()

    def compute(k):
        zs = zpeer(k)
        for j in range(nx):
            arrived(xs.at[zs, duo - 1 - c, xpeer(j)], r_d.at[zs, xpeer(j)])
        rows = duo * nx * slots
        block = xs[zs, :, :, :, pl.ds(0, d)].reshape(rows, d)
        side = xs[zs, :, :, :, pl.ds(d, MARK)].reshape(rows, MARK).astype(f32)
        lanes = lax.broadcasted_iota(jnp.int32, (rows, MARK), 1)
        held, width = w_g.shape[0], w_g.shape[2]
        for e in range(held):
            a = jnp.dot(block, w_g[e], preferred_element_type=f32)
            b = jnp.dot(block, w_u[e], preferred_element_type=f32)
            i = c * held + e
            w = jnp.sum(jnp.where((lanes == i) | (lanes == i + GROUP_SIZE), side, 0.0), axis=-1, keepdims=True)
            hid[:, pl.ds(e * width, width)] = (a / (1.0 + jnp.exp(-a)) * b * w).astype(bf16)
        po[zs] = jnp.dot(hid[...], w_d[...], preferred_element_type=f32).astype(bf16).reshape(duo, nx, slots, d)
        pair(k).start()

    def step(t, _):
        @pl.when(t < nz)
        def _():
            zs = zpeer(t)

            @pl.when(t > 0)
            def _():
                arrived(xs.at[zs, c, x], r_z.at[zs])

            for j in range(1, nx):
                fwd_x(t, j).start()
            fwd_d(t, 0).start()

        @pl.when((t >= 1) & (t < nz + 1))
        def _():
            k = t - 1
            for j in range(1, nx):
                arrived(xs.at[zpeer(k), c, xpeer(j)], r_x.at[zpeer(k), xpeer(j)])
                fwd_d(k, j).start()

        @pl.when(t == 2)
        def _():
            mixer_project()
            for cp in loads[3:]:
                cp.wait()

        @pl.when(t == 3)
        def _():
            mixer_finish()

        @pl.when((t >= 2) & (t < nz + 2))
        def _():
            compute(t - 2)

        @pl.when((t >= 3) & (t < nz + 3))
        def _():
            k = t - 3
            zs = zpeer(k)
            arrived(rd.at[zs], r_o.at[zs])
            sx[zs] = (po[zs, c].astype(f32) + rd[zs].astype(f32)).astype(bf16)
            for j in range(1, nx):
                sum_x(k, j).start()

        @pl.when(t >= 4)
        def _():
            k = t - 4
            zs = zpeer(k)
            total = sx[zs, x].astype(f32)
            for j in range(1, nx):
                arrived(rx.at[zs, xpeer(j)], r_p.at[zs, xpeer(j)])
                total = total + rx[zs, xpeer(j)].astype(f32)

            @pl.when(k == 0)
            def _():
                ret[z] = total.astype(bf16)

            @pl.when(k > 0)
            def _():
                sz[zs] = total.astype(bf16)
                back(k).start()

        return 0

    lax.fori_loop(0, nz + 4, step, 0)

    total = mo[x].astype(f32)
    for j in range(1, nx):
        arrived(mr.at[xpeer(j)], r_q.at[xpeer(j)])
        total = total + mr[xpeer(j)].astype(f32)
    mixed[...] = total.astype(bf16)

    for k in range(1, nz):
        arrived(ret.at[zpeer(k)], r_b.at[zpeer(k)])
    moe[...] = jnp.dot(mark[...], ret[...].reshape(nz * slots, d), preferred_element_type=f32).astype(bf16)

    rim().wait_send()
    for j in range(1, nx):
        mix_x(j).wait_send()
        mix_out(j).wait_send()
    for k in range(nz):
        if k:
            send_z(k).wait_send()
            back(k).wait_send()
        pair(k).wait_send()
        for j in range(nx):
            fwd_d(k, j).wait_send()
            if j:
                fwd_x(k, j).wait_send()
                sum_x(k, j).wait_send()


def shards(
    mixer_tokens, mixer_gain, proj_in, pool_weight, pool_scale, proj_out,
    expert_tokens, expert_gain, expert_route, route_gate, expert_gate, expert_up, expert_down,
):
    own, d = mixer_tokens.shape
    held, _, width = expert_gate.shape
    nx = lax.axis_size("tp")
    duo = GROUP_SIZE // held
    nz = lax.axis_size("ep") // duo
    experts = held * lax.axis_size("ep")
    slots = (own * GROUP_SIZE // experts) * GROUP_SIZE // 2
    dims = (nz, duo, nx, slots, own, d)
    vmem, anyspace = pl.BlockSpec(memory_space=pltpu.VMEM), pl.BlockSpec(memory_space=pl.ANY)
    dma = pltpu.SemaphoreType.DMA
    down = expert_down.reshape(held * width, d)
    local = proj_in.shape[1]
    V = pltpu.VMEM
    scratch = [
        V(proj_in.shape, bf16), V(pool_weight.shape, bf16), V(proj_out.shape, bf16),
        V(expert_gate.shape, bf16), V(expert_up.shape, bf16), V(down.shape, bf16),
        V((own, d + MARK), bf16), V((own, nz * slots), bf16), V((nz, slots, d + MARK), bf16),
        V((nz, duo, nx, slots, d + MARK), bf16), V((duo * nx * slots, held * width), bf16),
        V((nz, duo, nx, slots, d), bf16), V((nz, nx, slots, d), bf16),
        V((nz, nx, slots, d), bf16), V((nz, nx, slots, d), bf16),
        V((nz, slots, d), bf16), V((nz, slots, d), bf16),
        V((nx, own, d), bf16), V((HALO + nx * own, local), bf16),
        V((nx, own, d), bf16), V((nx, own, d), bf16),
        dma((6,)), dma((nz,)), dma((nz,)),
        dma((nz, nx)), dma((nz, nx)), dma((nz, nx)), dma((nz, nx)),
        dma((nz,)), dma((nz,)), dma((nz, nx)), dma((nz, nx)), dma((nz,)), dma((nz,)),
        dma((nx,)), dma((nx,)), dma, dma, dma((nx,)), dma((nx,)),
    ]
    return pl.pallas_call(
        functools.partial(kernel, dims),
        out_shape=(
            jax.ShapeDtypeStruct((own, d), bf16),
            jax.ShapeDtypeStruct((own, d), bf16),
        ),
        in_specs=[
            vmem, vmem, anyspace, anyspace, vmem, anyspace,
            vmem, vmem, vmem, vmem, anyspace, anyspace, anyspace,
        ],
        out_specs=(vmem, vmem),
        scratch_shapes=scratch,
        compiler_params=pltpu.CompilerParams(
            collective_id=0, has_side_effects=True, vmem_limit_bytes=62 * 1024 * 1024,
        ),
    )(
        mixer_tokens, mixer_gain.reshape(1, d), proj_in, pool_weight, pool_scale.reshape(1, local), proj_out,
        expert_tokens, expert_gain.reshape(1, d), expert_route, route_gate, expert_gate, expert_up, down,
    )


def solution(mesh):
    return jax.shard_map(
        shards,
        mesh=mesh,
        in_specs=(
            P(("grp", "ep", "tp"), None),
            P(),
            P(None, "tp"),
            P("tp", None, None),
            P("tp"),
            P("tp", None),
            P(("grp", "ep", "tp"), None),
            P(),
            P(("grp", "ep"), None),
            P(("grp", "ep"), None),
            P("ep", None, "tp"),
            P("ep", None, "tp"),
            P("ep", "tp", None),
        ),
        out_specs=(P(("grp", "ep", "tp"), None), P(("grp", "ep", "tp"), None)),
        check_vma=False,
    )
```

```python
import functools

import jax
import jax.numpy as jnp
from jax import lax
from jax.experimental import pallas as pl
from jax.experimental.pallas import tpu as pltpu
from jax.sharding import PartitionSpec as P

GROUP_SIZE = 4
MARK = 128
HALO = 16
PARTS = 2

norm_eps = 1e-05
MESH = pl.DeviceIdType.MESH
f32, bf16 = jnp.float32, jnp.bfloat16


def norm_rows(src, gain, store, step=16):
    def body(i, _):
        rows = pl.ds(pl.multiple_of(i * step, step), step)
        v = src[rows, :].astype(f32)
        center = jnp.mean(v, axis=-1, keepdims=True)
        v = v - center
        spread = jnp.mean(jnp.square(v), axis=-1, keepdims=True)
        store(rows, (v * lax.rsqrt(spread + norm_eps) * gain[...]).astype(bf16))
        return 0

    lax.fori_loop(0, src.shape[0] // step, body, 0)


def kernel(
    dims,
    mixer, mgain, proj_in, pool_w, pool_s, proj_out,
    tokens, egain, route, gate, wgate, wup, wdown,
    mixed, moe,
    w_in, w_pool, w_out, w_g, w_u, w_d,
    turn, aug, mark, out, xs, hid, po, rd, sx, rx, sz, ret,
    mx, ext, mo, mr,
    s_w, s_z, r_z, s_x, r_x, s_d, r_d, s_o, r_o, s_p, r_p, s_b, r_b,
    s_m, r_m, s_h, r_h, s_q, r_q,
):
    nz, parts, duo, nx, slots, own, d = dims
    units = nz * parts
    ep, x = lax.axis_index("ep"), lax.axis_index("tp")
    n_ep = nz * duo
    z, c = ep // duo, lax.rem(ep, duo)
    mate = z * duo + (duo - 1 - c)
    nxt, prv = lax.rem(ep + 1, n_ep), lax.rem(ep + n_ep - 1, n_ep)

    def xpeer(k):
        return lax.rem(x + k, nx)

    def zpeer(k):
        return lax.rem(z + k, nz)

    def unit(k):
        return zpeer(k // parts) * parts + lax.rem(k, parts)

    def mine(k):
        return z * parts + lax.rem(k, parts)

    def remote(src, dst, ssem, rsem, e, t):
        return pltpu.make_async_remote_copy(
            src_ref=src, dst_ref=dst, send_sem=ssem, recv_sem=rsem,
            device_id={"ep": e, "tp": t}, device_id_type=MESH)

    loads = [
        pltpu.make_async_copy(a, b, s_w.at[i])
        for i, (a, b) in enumerate(
            [(proj_in, w_in), (pool_w, w_pool), (proj_out, w_out), (wgate, w_g), (wup, w_u), (wdown, w_d)])
    ]
    for cp in loads:
        cp.start()

    barrier = pltpu.get_barrier_semaphore()

    def greet(e, t):
        pl.semaphore_signal(barrier, inc=1, device_id={"ep": e, "tp": t}, device_id_type=MESH)

    for k in range(1, nz):
        greet(zpeer(k) * duo + c, x)
    for k in range(1, nx):
        greet(ep, xpeer(k))
    greet(mate, x)
    greet(nxt, x)
    greet(prv, x)

    def send_z(k):
        g = zpeer(nz - k // parts)
        piece = g * parts + lax.rem(k, parts)
        return remote(out.at[piece], xs.at[mine(k), c, x], s_z.at[k], r_z.at[mine(k)], g * duo + c, x)

    def fwd_x(k, j):
        zs = unit(k)
        return remote(xs.at[zs, c, x], xs.at[zs, c, x], s_x.at[k, j], r_x.at[zs, x], ep, xpeer(j))

    def fwd_d(k, j):
        zs, xp = unit(k), xpeer(j)
        return remote(xs.at[zs, c, xp], xs.at[zs, c, xp], s_d.at[k, j], r_d.at[zs, xp], mate, x)

    def pair(k):
        zs = unit(k)
        return remote(po.at[zs, duo - 1 - c], rd.at[zs], s_o.at[k], r_o.at[zs], mate, x)

    def sum_x(k, j):
        zs, xp = unit(k), xpeer(j)
        return remote(sx.at[zs, xp], rx.at[zs, x], s_p.at[k, j], r_p.at[zs, x], ep, xp)

    def back(k):
        zs = unit(k)
        return remote(sz.at[zs], ret.at[mine(k)], s_b.at[k], r_b.at[mine(k)], zpeer(k // parts) * duo + c, x)

    def mix_x(j):
        return remote(mx.at[x], mx.at[x], s_m.at[j], r_m.at[x], ep, xpeer(j))

    def rim():
        return remote(ext.at[pl.ds(nx * own, HALO)], ext.at[pl.ds(0, HALO)], s_h, r_h, nxt, x)

    def mix_out(j, h):
        xp, half = xpeer(j), pl.ds(h * (own // 2), own // 2)
        return remote(mo.at[xp, half], mr.at[x, half], s_q.at[j, h], r_q.at[x, h], ep, xp)

    def arrived(dst, rsem):
        remote(dst, dst, s_h, rsem, ep, xpeer(1)).wait_recv()

    def keep_mixer(rows, v):
        mx[x, rows, :] = v

    norm_rows(mixer, mgain, keep_mixer)
    pl.semaphore_wait(barrier, nz - 1 + nx - 1 + 3)
    for j in range(1, nx):
        mix_x(j).start()

    def keep_tokens(rows, v):
        aug[rows, pl.ds(0, d)] = v

    norm_rows(tokens, egain, keep_tokens)
    base = pl.ds(pl.multiple_of(x * own, own), own)
    turn[...] = jnp.zeros_like(turn)
    turn[0:2, :] = route[:, base].astype(f32)
    turn[2:4, :] = gate[:, base]
    columns = turn[...].T
    lane = lax.broadcasted_iota(jnp.int32, (own, MARK), 1)
    r0, r1 = columns[:, 0:1].astype(jnp.int32), columns[:, 1:2].astype(jnp.int32)
    i0, i1 = lax.rem(r0, GROUP_SIZE), lax.rem(r1, GROUP_SIZE)
    g0, g1 = columns[:, 2:3], columns[:, 3:4]
    head = jnp.where(lane == i0, g0, 0.0) + jnp.where(lane == i1, g1, 0.0)
    tail = jnp.where(lane == i0 + GROUP_SIZE, g0, 0.0) + jnp.where(lane == i1 + GROUP_SIZE, g1, 0.0)
    rest = tail - tail.astype(bf16).astype(f32)
    aug[:, pl.ds(d, MARK)] = (head + rest).astype(bf16)
    member = (lane == r0 // GROUP_SIZE).astype(f32)
    row = lax.broadcasted_iota(jnp.int32, (own, own), 0)
    col = lax.broadcasted_iota(jnp.int32, (own, own), 1)
    before = jnp.dot((col < row).astype(f32).astype(bf16), member.astype(bf16), preferred_element_type=f32)
    place = jnp.sum(member * (before + (lane * (parts * slots)).astype(f32)), axis=-1, keepdims=True).astype(jnp.int32)
    slot = lax.broadcasted_iota(jnp.int32, (own, units * slots), 1)
    mark[...] = (slot == place).astype(f32).astype(bf16)
    packed = lax.dot_general(
        mark[...], aug[...], (((0,), (0,)), ((), ())), preferred_element_type=f32
    ).astype(bf16)
    out[...] = packed.reshape(units, slots, d + MARK)

    for k in range(parts, units):
        send_z(k).start()
    for k in range(parts):
        xs[mine(k), c, x] = out[mine(k)]

    def mixer_project():
        for j in range(1, nx):
            arrived(mx.at[xpeer(j)], r_m.at[xpeer(j)])
        loads[0].wait()
        rows = mx[...].reshape(nx * own, d)
        ext[pl.ds(HALO, nx * own), :] = jnp.dot(rows, w_in[...], preferred_element_type=f32).astype(bf16)
        rim().start()

    def mixer_finish():
        arrived(ext.at[pl.ds(0, HALO)], r_h)
        loads[1].wait()
        loads[2].wait()
        groups, width = w_pool.shape[0], w_pool.shape[1]
        rows = nx * own
        at = ep * rows + lax.broadcasted_iota(jnp.int32, (rows, width), 0)
        total = None
        for g in range(groups):
            cols = pl.ds(g * width, width)
            v = ext[:, cols].astype(f32)
            r = lax.broadcasted_iota(jnp.int32, v.shape, 0)
            v = jnp.where((r < HALO) & (ep == 0), 0.0, v)
            group = x * groups + g
            s, window, picked = v, 1, None
            for level in range(groups * nx):
                s = s + pltpu.roll(s, window, 0)
                window *= 2
                picked = s if picked is None else jnp.where(group == level, s, picked)
            w = lax.shift_left(jnp.int32(2), group)
            covered = jnp.minimum(at + 1, w).astype(f32)
            diff = (picked[HALO:] / covered - v[HALO:]).astype(bf16)
            m = jnp.dot(diff, w_pool[g], preferred_element_type=f32) * pool_s[:, cols]
            part = jnp.dot(m.astype(bf16), w_out[cols, :], preferred_element_type=f32)
            total = part if total is None else total + part
        mo[...] = total.astype(bf16).reshape(nx, own, d)

    def compute(k):
        zs = unit(k)
        for j in range(nx):
            arrived(xs.at[zs, duo - 1 - c, xpeer(j)], r_d.at[zs, xpeer(j)])
        rows = duo * nx * slots
        block = xs[zs, :, :, :, pl.ds(0, d)].reshape(rows, d)
        side = xs[zs, :, :, :, pl.ds(d, MARK)].reshape(rows, MARK).astype(f32)
        lanes = lax.broadcasted_iota(jnp.int32, (rows, MARK), 1)
        held, width = w_g.shape[0], w_g.shape[2]
        for e in range(held):
            a = jnp.dot(block, w_g[e], preferred_element_type=f32)
            b = jnp.dot(block, w_u[e], preferred_element_type=f32)
            i = c * held + e
            w = jnp.sum(jnp.where((lanes == i) | (lanes == i + GROUP_SIZE), side, 0.0), axis=-1, keepdims=True)
            hid[:, pl.ds(e * width, width)] = (a / (1.0 + jnp.exp(-a)) * b * w).astype(bf16)
        po[zs] = jnp.dot(hid[...], w_d[...], preferred_element_type=f32).astype(bf16).reshape(duo, nx, slots, d)
        pair(k).start()

    def step(t, _):
        @pl.when(t < units)
        def _():
            zs = unit(t)

            @pl.when(t >= parts)
            def _():
                arrived(xs.at[zs, c, x], r_z.at[zs])

            for j in range(1, nx):
                fwd_x(t, j).start()
            fwd_d(t, 0).start()

        @pl.when((t >= 1) & (t < units + 1))
        def _():
            k = t - 1
            for j in range(1, nx):
                arrived(xs.at[unit(k), c, xpeer(j)], r_x.at[unit(k), xpeer(j)])
                fwd_d(k, j).start()

        @pl.when((t >= 3) & (t < units + 3))
        def _():
            k = t - 3
            zs = unit(k)
            arrived(rd.at[zs], r_o.at[zs])
            sx[zs] = (po[zs, c].astype(f32) + rd[zs].astype(f32)).astype(bf16)
            for j in range(1, nx):
                sum_x(k, j).start()

            @pl.when(k == units - 2)
            def _():
                for j in range(1, nx):
                    mix_out(j, 0).start()

            @pl.when(k == units - 1)
            def _():
                for j in range(1, nx):
                    mix_out(j, 1).start()

        @pl.when(t >= 4)
        def _():
            k = t - 4
            zs = unit(k)
            total = sx[zs, x].astype(f32)
            for j in range(1, nx):
                arrived(rx.at[zs, xpeer(j)], r_p.at[zs, xpeer(j)])
                total = total + rx[zs, xpeer(j)].astype(f32)

            @pl.when(k < parts)
            def _():
                ret[zs] = total.astype(bf16)

            @pl.when(k >= parts)
            def _():
                sz[zs] = total.astype(bf16)
                back(k).start()

        @pl.when(t == units // 2)
        def _():
            mixer_project()

        @pl.when(t == units // 2 + 1)
        def _():
            mixer_finish()

        @pl.when(t == 2)
        def _():
            for cp in loads[3:]:
                cp.wait()

        @pl.when((t >= 2) & (t < units + 2))
        def _():
            compute(t - 2)

        return 0

    lax.fori_loop(0, units + 4, step, 0)

    total = mo[x].astype(f32)
    for j in range(1, nx):
        for h in range(2):
            half = pl.ds(h * (own // 2), own // 2)
            arrived(mr.at[xpeer(j), half], r_q.at[xpeer(j), h])
        total = total + mr[xpeer(j)].astype(f32)
    mixed[...] = total.astype(bf16)

    for k in range(parts, units):
        arrived(ret.at[unit(k)], r_b.at[unit(k)])
    moe[...] = jnp.dot(mark[...], ret[...].reshape(units * slots, d), preferred_element_type=f32).astype(bf16)

    rim().wait_send()
    for j in range(1, nx):
        mix_x(j).wait_send()
        mix_out(j, 0).wait_send()
        mix_out(j, 1).wait_send()
    for k in range(units):
        if k >= parts:
            send_z(k).wait_send()
            back(k).wait_send()
        pair(k).wait_send()
        for j in range(nx):
            fwd_d(k, j).wait_send()
            if j:
                fwd_x(k, j).wait_send()
                sum_x(k, j).wait_send()


def shards(
    mixer_tokens, mixer_gain, proj_in, pool_weight, pool_scale, proj_out,
    expert_tokens, expert_gain, expert_route, route_gate, expert_gate, expert_up, expert_down,
):
    own, d = mixer_tokens.shape
    held, _, width = expert_gate.shape
    nx = lax.axis_size("tp")
    duo = GROUP_SIZE // held
    nz = lax.axis_size("ep") // duo
    experts = held * lax.axis_size("ep")
    slots = (own * GROUP_SIZE // experts) * GROUP_SIZE // 2
    parts = PARTS if slots % (PARTS * 16) == 0 else 1
    units, slots = nz * parts, slots // parts
    dims = (nz, parts, duo, nx, slots, own, d)
    vmem, anyspace = pl.BlockSpec(memory_space=pltpu.VMEM), pl.BlockSpec(memory_space=pl.ANY)
    dma = pltpu.SemaphoreType.DMA
    down = expert_down.reshape(held * width, d)
    local = proj_in.shape[1]
    V = pltpu.VMEM
    scratch = [
        V(proj_in.shape, bf16), V(pool_weight.shape, bf16), V(proj_out.shape, bf16),
        V(expert_gate.shape, bf16), V(expert_up.shape, bf16), V(down.shape, bf16),
        V((own, own), f32), V((own, d + MARK), bf16), V((own, units * slots), bf16), V((units, slots, d + MARK), bf16),
        V((units, duo, nx, slots, d + MARK), bf16), V((duo * nx * slots, held * width), bf16),
        V((units, duo, nx, slots, d), bf16), V((units, nx, slots, d), bf16),
        V((units, nx, slots, d), bf16), V((units, nx, slots, d), bf16),
        V((units, slots, d), bf16), V((units, slots, d), bf16),
        V((nx, own, d), bf16), V((HALO + nx * own, local), bf16),
        V((nx, own, d), bf16), V((nx, own, d), bf16),
        dma((6,)), dma((units,)), dma((units,)),
        dma((units, nx)), dma((units, nx)), dma((units, nx)), dma((units, nx)),
        dma((units,)), dma((units,)), dma((units, nx)), dma((units, nx)), dma((units,)), dma((units,)),
        dma((nx,)), dma((nx,)), dma, dma, dma((nx, 2)), dma((nx, 2)),
    ]
    return pl.pallas_call(
        functools.partial(kernel, dims),
        out_shape=(
            jax.ShapeDtypeStruct((own, d), bf16),
            jax.ShapeDtypeStruct((own, d), bf16),
        ),
        in_specs=[
            vmem, vmem, anyspace, anyspace, vmem, anyspace,
            vmem, vmem, vmem, vmem, anyspace, anyspace, anyspace,
        ],
        out_specs=(vmem, vmem),
        scratch_shapes=scratch,
        compiler_params=pltpu.CompilerParams(
            collective_id=0, has_side_effects=True, vmem_limit_bytes=62 * 1024 * 1024,
        ),
    )(
        mixer_tokens, mixer_gain.reshape(1, d), proj_in, pool_weight, pool_scale.reshape(1, local), proj_out,
        expert_tokens, expert_gain.reshape(1, d), expert_route.T, route_gate.T, expert_gate, expert_up, down,
    )


def solution(mesh):
    return jax.shard_map(
        shards,
        mesh=mesh,
        in_specs=(
            P(("grp", "ep", "tp"), None),
            P(),
            P(None, "tp"),
            P("tp", None, None),
            P("tp"),
            P("tp", None),
            P(("grp", "ep", "tp"), None),
            P(),
            P(("grp", "ep"), None),
            P(("grp", "ep"), None),
            P("ep", None, "tp"),
            P("ep", None, "tp"),
            P("ep", "tp", None),
        ),
        out_specs=(P(("grp", "ep", "tp"), None), P(("grp", "ep", "tp"), None)),
        check_vma=False,
    )
```
